32 devices in a mesh: ep: 16 (over z, y, x), tp: 2 (over core).
Axes of the slice: x: 2, y: 2, z: 4, core: 2. Of those that a mesh axis runs over, the one named last changes fastest.
Arguments:
- tokens: bfloat16 [6144, 3072], P('ep', 'tp'), may hold values from -6 to 6
- cotangent: bfloat16 [6144, 3072], P('ep', 'tp'), may hold values from -6 to 6
- experts: int32 [6144, 2], P('ep'), may hold values from 0 to 15, all different within a row; in each aligned block of 384 rows (0 to 383, 384 to 767, ...) at most 72 rows name the same one
- gate: float32 [6144, 2], P('ep'), may hold values from 0.2 to 1
- w_gate: bfloat16 [16, 3072, 768], P('ep', None, 'tp'), may hold values from -0.109375 to 0.109375
- w_up: bfloat16 [16, 3072, 768], P('ep', None, 'tp'), may hold values from -0.109375 to 0.109375
- w_down: bfloat16 [16, 768, 3072], P('ep', 'tp'), may hold values from -0.21875 to 0.21875
Outputs:
- token_grad: bfloat16 [6144, 3072], P('ep', 'tp')
- gate_grad: float32 [6144, 2], P('ep')
- gate_weight_grad: bfloat16 [16, 3072, 768], P('ep', None, 'tp')
- up_weight_grad: bfloat16 [16, 3072, 768], P('ep', None, 'tp')
- down_weight_grad: bfloat16 [16, 768, 3072], P('ep', 'tp')
- gate_row_norms: float32 [16, 3072], P('ep')
- up_row_norms: float32 [16, 3072], P('ep')
- down_row_norms: float32 [16, 768], P('ep', 'tp')
The draws below stay inside these ranges and needn't reach their ends.
Inputs may be any that keep to these rules, and one draw needn't show every extreme that they name: A row names 2 different experts. In each aligned block of 384 rows (the rows of one index of ep) no expert is named by more than 72 rows, a bound that some block reaches.
All inputs are finite; a program needn't handle non-finite values.
Results may differ from the reference program's by a relative error of at most 0.008.
Values may be sent and summed in bfloat16 or wider, within the bound.
A program may use at most 128 MiB of HBM per device.

```python
import math
import jax
import jax.numpy as jnp
import numpy as np
from jax import lax

D = 3072
F = 768
TOP = 2
TOK_EP = 384
EXPERTS = 16
CAP = 72
TOKENS = 6144
N_EP = 16
N_TP = 2


def shard_levels(own_key, extent, cuts, low, high):
    def one(position, blocks):
        steps = jax.random.uniform(jax.random.fold_in(jax.random.fold_in(own_key, 6), position), (blocks,), jnp.float32, low / len(cuts), high / len(cuts))
        return jnp.repeat(jnp.exp(steps), extent[position] // blocks).reshape((-1,) + (1,) * (len(extent) - position - 1))

    loudness = one(*cuts[0])
    for cut in cuts[1:]:
        loudness = loudness * one(*cut)
    return loudness


def deal_out(own_key, own, number, rows, amount, top, limit, slope):
    order = jax.random.permutation(own_key, amount)
    packed, ordinary = portions_of(amount, rows * top, limit, slope, True), portions_of(amount, rows * top, limit, slope, False)
    places = jnp.arange(amount)

    def named(lengths, offset_by):
        used = int((lengths > 0).sum())
        fixed = max(1, used // 4)
        moved = fixed + (places - fixed + offset_by * (used - fixed)) % max(1, amount - fixed)
        return jnp.zeros((amount,), jnp.int32).at[order[jnp.where(places < fixed, places, moved)]].set(jnp.asarray(lengths, jnp.int32))

    lengths = jnp.where(number % 4 == 0, named(packed, number // 4), named(ordinary, number - number // 4 - 1))
    mixed = jax.random.permutation(jax.random.fold_in(own, 3), amount)
    donor, taker = mixed[0:amount // 2 * 2:2], mixed[1:amount // 2 * 2:2]
    margin = jnp.minimum(lengths[donor] - 1, limit - lengths[taker]) // 2
    margin = jnp.where((donor == order[0]) | (taker == order[0]) | (lengths[taker] == 0), 0, jnp.maximum(margin, 0))
    moved = jax.random.randint(jax.random.fold_in(own, 4), (amount // 2,), 0, 1 << 20) % (margin + 1)
    lengths = lengths.at[donor].add(-moved).at[taker].add(moved)
    members = jnp.searchsorted(jnp.cumsum(lengths), jnp.arange(rows * top), side="right").astype(jnp.int32)
    listing = members.reshape(top, rows).T
    listing = listing[jax.random.permutation(jax.random.fold_in(own, 1), rows)]
    offset_by = jax.random.randint(jax.random.fold_in(own, 2), (rows, 1), 0, top)
    return jnp.take_along_axis(listing, (jnp.arange(top)[None, :] + offset_by) % top, axis=1)


def portions_of(count, total, reach, lean, full):
    portions = [(1 << 20) // math.isqrt(grade ** lean) + 1 for grade in range(1, count + 1)]
    largest = reach if full else min(reach, max(-(-total // count), total * portions[0] // sum(portions)))
    least = 1 if total - largest >= count - 1 else 0
    holding, spare = [largest] + [least] * (count - 1), total - largest - least * (count - 1)
    while spare > 0:
        candidates = [i for i in range(1, count) if holding[i] < largest] or [i for i in range(1, count) if holding[i] < reach]
        mass, budget = sum([portions[i] for i in candidates]), spare
        for i in candidates:
            addition = min(reach - holding[i], max(1, budget * portions[i] // mass), spare)
            holding[i] = holding[i] + addition
            spare = spare - addition
    return np.array(holding)


def centred(stream_key, shape, deviation, most, split=(), held_as=jnp.bfloat16):
    entries = jax.random.normal(stream_key, shape, jnp.float32) * deviation
    if len(split) > 0:
        entries = shard_levels(stream_key, shape, split, -0.22, 0.18) * entries
    return jnp.clip(entries, min=-most, max=most).astype(held_as)


def setup_inputs(seed: int = 0) -> dict:
    seeds = jax.random.split(jax.random.key(seed), 8)
    tokens = centred(seeds[0], (TOKENS, D), 1.0, 6.0, ((0, 16), (1, 2)))
    cotangent = centred(seeds[1], (TOKENS, D), 1.0, 6.0, ((0, 16), (1, 2)))
    experts_keys = jax.random.split(jax.random.fold_in(seeds[2], 1), TOKENS // TOK_EP)
    experts_turns = jax.random.permutation(jax.random.fold_in(seeds[2], 3), TOKENS // TOK_EP)
    experts = jax.vmap(lambda own, number: deal_out(jax.random.fold_in(seeds[2], 2), own, number, TOK_EP, EXPERTS, TOP, CAP, 2))(experts_keys, experts_turns).reshape((TOKENS, TOP))
    gate = jnp.clip(0.2 + 0.8 * jax.random.uniform(seeds[3], (TOKENS, TOP), jnp.float32) ** shard_levels(seeds[3], (TOKENS, TOP), ((0, 16),), -0.2, 0.2), 0.2, 1.0)
    w_gate = centred(seeds[4], (EXPERTS, D, F), D ** -0.5, 0.109375, ((0, 16), (2, 2)))
    w_up = centred(seeds[5], (EXPERTS, D, F), D ** -0.5, 0.109375, ((0, 16), (2, 2)))
    w_down = centred(seeds[6], (EXPERTS, F, D), F ** -0.5, 0.21875, ((0, 16), (1, 2)))
    return dict(tokens=tokens, cotangent=cotangent, experts=experts, gate=gate, w_gate=w_gate, w_up=w_up, w_down=w_down)


def slot_table(route_block, experts_count, cap):
    pair_ids = route_block.reshape(-1).astype(jnp.int32)
    pair_count = pair_ids.shape[0]
    onehot = (pair_ids[:, None] == jnp.arange(experts_count, dtype=jnp.int32)[None, :]).astype(jnp.int32)
    ranking = jnp.sum(jnp.cumsum(onehot, axis=0) * onehot, axis=1) - 1
    slot_of = (pair_ids * cap + ranking).astype(jnp.int32)
    slot_pairs = jnp.full((experts_count * cap,), pair_count, jnp.int32).at[slot_of].set(
        jnp.arange(pair_count, dtype=jnp.int32))
    return slot_of, slot_pairs


def expert_terms(rows_in, rows_cot, gate_mat, up_mat, down_mat):
    contract_last = (((1,), (1,)), ((), ()))
    contract_rows = (((0,), (0,)), ((), ()))
    gate_pre = jnp.dot(rows_in, gate_mat, preferred_element_type=jnp.float32)
    up_pre = jnp.dot(rows_in, up_mat, preferred_element_type=jnp.float32)
    sigma = jax.nn.sigmoid(gate_pre)
    active = gate_pre * sigma
    hidden = (active * up_pre).astype(jnp.bfloat16)
    hidden_grad = lax.dot_general(rows_cot, down_mat, contract_last, preferred_element_type=jnp.float32)
    products = jnp.sum(hidden.astype(jnp.float32) * hidden_grad, axis=1).astype(jnp.bfloat16)
    gate_grad_pre = (hidden_grad * up_pre * sigma * (1.0 + gate_pre * (1.0 - sigma))).astype(jnp.bfloat16)
    up_grad_pre = (hidden_grad * active).astype(jnp.bfloat16)
    block = F // N_TP
    total = jnp.zeros((rows_in.shape[0], D), jnp.float32)
    for index in range(N_TP):
        lower = index * block
        upper = lower + block
        piece = lax.dot_general(gate_grad_pre[:, lower:upper], gate_mat[:, lower:upper], contract_last,
                                preferred_element_type=jnp.float32)
        piece = piece + lax.dot_general(up_grad_pre[:, lower:upper], up_mat[:, lower:upper], contract_last,
                                        preferred_element_type=jnp.float32)
        rounded = lax.optimization_barrier(piece.astype(jnp.bfloat16))
        total = total + rounded.astype(jnp.float32)
    route_rows = total.astype(jnp.bfloat16)
    gate_sum = lax.dot_general(rows_in, gate_grad_pre, contract_rows, preferred_element_type=jnp.float32)
    up_sum = lax.dot_general(rows_in, up_grad_pre, contract_rows, preferred_element_type=jnp.float32)
    down_sum = lax.dot_general(hidden, rows_cot, contract_rows, preferred_element_type=jnp.float32)
    return (route_rows, products, gate_sum.astype(jnp.bfloat16), up_sum.astype(jnp.bfloat16),
            down_sum.astype(jnp.bfloat16), jnp.sum(gate_sum * gate_sum, axis=1),
            jnp.sum(up_sum * up_sum, axis=1), jnp.sum(down_sum * down_sum, axis=1))


def reference(tokens, cotangent, experts, gate, w_gate, w_up, w_down):
    pair_total = TOKENS * TOP
    pair_block = TOK_EP * TOP
    routes = experts.reshape(N_EP, TOK_EP, TOP)
    slot_of, slot_pairs = jax.vmap(lambda block_routes: slot_table(block_routes, EXPERTS, CAP))(routes)
    offsets = (jnp.arange(N_EP, dtype=jnp.int32) * pair_block)[:, None]
    global_pairs = jnp.where(slot_pairs < pair_block, slot_pairs + offsets, pair_total).astype(jnp.int32)
    by_expert = global_pairs.reshape(N_EP, EXPERTS, CAP).transpose(1, 0, 2).reshape(EXPERTS, N_EP * CAP)
    weighted = (gate[:, :, None] * cotangent.astype(jnp.float32)[:, None, :]).astype(jnp.bfloat16)
    padding = jnp.zeros((1, D), jnp.bfloat16)
    token_pad = jnp.concatenate([tokens, padding], axis=0)
    weighted_pad = jnp.concatenate([weighted.reshape(pair_total, D), padding], axis=0)

    def per_expert(operands):
        indices, gate_mat, up_mat, down_mat = operands
        rows_in = token_pad[indices // TOP]
        rows_cot = weighted_pad[indices]
        return expert_terms(rows_in, rows_cot, gate_mat, up_mat, down_mat)

    results = lax.map(per_expert, (by_expert, w_gate, w_up, w_down))
    route_rows, products = results[0], results[1]
    flat_index = by_expert.reshape(-1)
    pair_rows = jnp.zeros((pair_total + 1, D), jnp.bfloat16).at[flat_index].set(route_rows.reshape(-1, D))
    pair_products = jnp.zeros((pair_total + 1,), jnp.bfloat16).at[flat_index].set(products.reshape(-1))
    token_grad = jnp.sum(pair_rows[:pair_total].astype(jnp.float32).reshape(TOKENS, TOP, D), axis=1)
    gate_grad = pair_products[:pair_total].astype(jnp.float32).reshape(TOKENS, TOP) / gate
    return (token_grad.astype(jnp.bfloat16), gate_grad, results[2], results[3], results[4],
            results[5], results[6], results[7])
```

```python
import functools
import jax
import jax.numpy as jnp
from jax import lax
from jax.experimental import pallas as pl
from jax.experimental.pallas import tpu as pltpu
from jax.sharding import PartitionSpec as P

F32 = jnp.float32
BF16 = jnp.bfloat16
LAST = (((1,), (1,)), ((), ()))
ROWS = (((0,), (0,)), ((), ()))
OWN = 0


def slots_of(routes, groups, cap):
    rows = routes.shape[1]
    ids = lax.broadcasted_iota(jnp.int32, (groups, rows), 0)
    hits = [routes[k][None, :] == ids for k in range(routes.shape[0])]
    named = sum(h.astype(F32) for h in hits).astype(BF16)
    before = (
        lax.broadcasted_iota(jnp.int32, (rows, rows), 0)
        < lax.broadcasted_iota(jnp.int32, (rows, rows), 1)
    ).astype(BF16)
    rank = jnp.dot(named, before, preferred_element_type=F32)
    return jnp.stack(
        [routes[k] * cap + jnp.sum(jnp.where(h, rank, 0.0), axis=0).astype(jnp.int32) for k, h in enumerate(hits)]
    )


def wide(width):
    for step in (512, 384, 256, 128):
        if width % step == 0:
            return step
    return width


def forward_kernel(
    n, cap, tok_ref, cot_ref, meta_ref, tok_out, cot_out,
    held, relay, hmeta, rmeta, snd, rows, pick, slot_gate,
    held_send, held_recv, relay_send, relay_recv, pass_send, meta_sem,
    own_send, own_recv, far_send, far_recv, pair_send, pair_recv, out_sem,
):
    rows_t, width = tok_ref.shape
    half_n, quarter = n // 2, n // 4
    me, core = lax.axis_index("ep"), lax.axis_index("tp")
    plane, xy = me // quarter, me % quarter
    side, spot = me // half_n, me % half_n
    outer = jnp.logical_or(plane == 0, plane == 3)
    inner = jnp.logical_not(outer)
    cross = jnp.where(plane == 1, 2, 1) * quarter + xy
    own_inner = (1 + side) * quarter + xy
    near_base = (2 - side) * quarter
    far_base = 3 * (1 - side) * quarter
    columns = pl.ds(pl.multiple_of(core * width, width), width)
    source = (tok_ref, cot_ref)
    blocks = half_n * cap

    def remote(src, dst, send, recv, ep, tp=None):
        return pltpu.make_async_remote_copy(
            src_ref=src, dst_ref=dst, send_sem=send, recv_sem=recv,
            device_id={"ep": ep, "tp": core if tp is None else tp},
            device_id_type=pl.DeviceIdType.MESH,
        )

    barrier = pltpu.get_barrier_semaphore()

    def greet(ep, tp):
        pl.semaphore_signal(barrier, inc=1, device_id={"ep": ep, "tp": tp}, device_id_type=pl.DeviceIdType.MESH)

    for s in range(1, half_n):
        greet(side * half_n + (spot + s) % half_n, core)
    greet(me, 1 - core)

    @pl.when(inner)
    def _():
        greet(cross, core)
        pl.semaphore_wait(barrier, half_n + 1)

    @pl.when(outer)
    def _():
        pl.semaphore_wait(barrier, half_n)

    def near_copy(a):
        return remote(source[a], held.at[0, a], held_send.at[0, a], held_recv.at[0, a], cross)

    def relay_copy(a):
        return remote(source[a], relay.at[a], relay_send.at[a], relay_recv.at[a], own_inner)

    def pass_copy(a):
        return remote(relay.at[a], held.at[1, a], held_send.at[1, a], held_recv.at[1, a], cross)

    near_meta = remote(meta_ref, hmeta.at[0], meta_sem.at[0], meta_sem.at[1], cross)
    relay_meta = remote(meta_ref, rmeta, meta_sem.at[2], meta_sem.at[3], own_inner)
    pass_meta = remote(rmeta, hmeta.at[1], meta_sem.at[4], meta_sem.at[5], cross)

    def own_copy(a, s):
        target = (spot + s) % half_n
        return remote(
            snd.at[OWN, a, target], rows.at[a, me, :, columns],
            own_send.at[a, s], own_recv.at[a, s], side * half_n + target,
        )

    def far_copy(b, a, s, out):
        target = (xy + s) % quarter
        plane_to = 3 * side if out else 1 + side
        base = near_base if b == 0 else far_base
        return remote(
            snd.at[1 + b, a, (plane_to % 2) * quarter + target], rows.at[a, base + xy, :, columns],
            far_send.at[b, a, int(out), s], far_recv.at[b, a, s], plane_to * quarter + target,
        )

    def pair_copy(a, base, count, slot):
        block = rows.at[a, pl.ds(base, count), :, columns]
        return remote(block, block, pair_send.at[a, slot], pair_recv.at[a, slot], me, 1 - core)

    def make_pick(b, table):
        slot = table[0:2, :].astype(jnp.int32) - side * blocks
        ids = lax.broadcasted_iota(jnp.int32, (blocks, rows_t), 0)
        match = [slot[k:k + 1, :] == ids for k in range(2)]
        pick[b] = sum(m.astype(F32) for m in match).astype(BF16)
        slot_gate[b] = sum(
            jnp.sum(jnp.where(m, table[2 + k:3 + k, :], 0.0), axis=1, keepdims=True) for k, m in enumerate(match)
        )

    step = wide(width)

    def fill(b, a, src):
        @pl.loop(0, width // step)
        def _(c):
            cols = pl.ds(pl.multiple_of(c * step, step), step)
            block = jnp.dot(pick[b], src[:, cols], preferred_element_type=F32)
            if a == 1:
                block = block * slot_gate[b]
            snd[b, a, :, :, cols] = block.astype(BF16).reshape(half_n, cap, step)

    def place(b, a, group, where):
        rows[a, group, :, columns] = snd[b, a, where]

    @pl.when(inner)
    def _():
        near_meta.start()
        near_copy(0).start()
        near_copy(1).start()

    @pl.when(outer)
    def _():
        relay_meta.start()
        relay_copy(0).start()

    make_pick(OWN, meta_ref)
    for a in range(2):
        if a == 1:
            @pl.when(outer)
            def _():
                relay_copy(1).start()
        fill(OWN, a, source[a])
        for s in range(half_n - 1, 0, -1):
            own_copy(a, s).start()
        place(OWN, a, me, spot)

    def hand_on(b, a):
        fill(1 + b, a, held.at[b, a])
        for s in range(quarter):
            far_copy(b, a, s, True).start()
        for s in range(1, quarter):
            far_copy(b, a, s, False).start()
        place(1 + b, a, (near_base if b == 0 else far_base) + xy, (1 - side) * quarter + xy)

    def own_arrived(a):
        for s in range(1, half_n):
            own_copy(a, s).wait_recv()
        pair_copy(a, side * half_n, half_n, 0).start()

    def far_arrived(b, a):
        for s in range(1, quarter):
            far_copy(b, a, s, False).wait_recv()

        @pl.when(outer)
        def _():
            far_copy(b, a, 0, True).wait_recv()

        pair_copy(a, near_base if b == 0 else far_base, quarter, 1 + b).start()

    @pl.when(inner)
    def _():
        near_meta.wait_recv()
        relay_meta.wait_recv()
        pass_meta.start()
        make_pick(1, hmeta.at[0])
        relay_copy(0).wait_recv()
        pass_copy(0).start()
        near_copy(0).wait_recv()
        hand_on(0, 0)
        near_copy(1).wait_recv()
        hand_on(0, 1)
        pass_meta.wait_recv()
        make_pick(2, hmeta.at[1])
        relay_copy(1).wait_recv()
        pass_copy(1).start()
        pass_copy(0).wait_recv()
        hand_on(1, 0)

    own_arrived(0)
    far_arrived(0, 0)
    own_arrived(1)
    far_arrived(0, 1)

    @pl.when(inner)
    def _():
        pass_copy(1).wait_recv()
        hand_on(1, 1)

    far_arrived(1, 0)

    far_arrived(1, 1)

    spans = ((side * half_n, half_n), (near_base, quarter), (far_base, quarter))
    for a in range(2):
        for slot, (base, count) in enumerate(spans):
            pair_copy(a, base, count, slot).wait()
    outs = [pltpu.make_async_copy(rows.at[a], (tok_out, cot_out)[a], out_sem.at[a]) for a in range(2)]
    for o in outs:
        o.start()
    for a in range(2):
        for s in range(1, half_n):
            own_copy(a, s).wait_send()

    @pl.when(inner)
    def _():
        near_meta.wait_send()
        pass_meta.wait_send()
        for a in range(2):
            near_copy(a).wait_send()
            pass_copy(a).wait_send()
            for b in range(2):
                for s in range(quarter):
                    far_copy(b, a, s, True).wait_send()
                for s in range(1, quarter):
                    far_copy(b, a, s, False).wait_send()

    @pl.when(outer)
    def _():
        relay_meta.wait_send()
        for a in range(2):
            relay_copy(a).wait_send()

    for o in outs:
        o.wait()


def forward(n, cap, tokens, cotangent, meta):
    rows_t, width = tokens.shape
    half_n, quarter = n // 2, n // 4
    shape = jax.ShapeDtypeStruct((n, cap, 2 * width), BF16)
    dma = pltpu.SemaphoreType.DMA
    vm = pl.BlockSpec(memory_space=pltpu.VMEM)
    return pl.pallas_call(
        functools.partial(forward_kernel, n, cap),
        out_shape=(shape, shape),
        in_specs=[vm] * 3,
        out_specs=[pl.BlockSpec(memory_space=pl.ANY)] * 2,
        scratch_shapes=[
            pltpu.VMEM((2, 2, rows_t, width), BF16),
            pltpu.VMEM((2, rows_t, width), BF16),
            pltpu.VMEM((2,) + meta.shape, F32),
            pltpu.VMEM(meta.shape, F32),
            pltpu.VMEM((3, 2, half_n, cap, width), BF16),
            pltpu.VMEM((2, n, cap, 2 * width), BF16),
            pltpu.VMEM((3, half_n * cap, rows_t), BF16),
            pltpu.VMEM((3, half_n * cap, 1), F32),
            dma((2, 2)), dma((2, 2)), dma((2,)), dma((2,)), dma((2,)), dma((6,)),
            dma((2, half_n)), dma((2, half_n)), dma((2, 2, 2, quarter)), dma((2, 2, quarter)),
            dma((2, 3)), dma((2, 3)), dma((2,)),
        ],
        compiler_params=pltpu.CompilerParams(
            collective_id=0, has_side_effects=True, vmem_limit_bytes=60 * 1024 * 1024
        ),
        cost_estimate=pl.CostEstimate(flops=10**9, bytes_accessed=10**8, transcendentals=0),
    )(tokens, cotangent, meta)


def per_device(tokens, cotangent, experts, gate, w_gate, w_up, w_down):
    groups = lax.axis_size("ep")
    tok_rows, top = experts.shape
    cap = 3 * tok_rows * top // (2 * groups)
    cap = (cap + 7) // 8 * 8
    total = groups * cap
    half = tokens.shape[1]
    core = lax.axis_index("tp")
    swap = [(0, 1), (1, 0)]
    slot = slots_of(experts.T, groups, cap)
    gate_t = gate.T
    meta = jnp.concatenate([slot.astype(F32), gate_t, jnp.zeros((4, tok_rows), F32)], axis=0)
    rows_in, rows_cot = forward(groups, cap, tokens, cotangent, meta)
    rows_in, rows_cot = rows_in.reshape(total, 2 * half), rows_cot.reshape(total, 2 * half)
    slot_ids = lax.broadcasted_iota(jnp.int32, (total, tok_rows), 0)
    match = [slot[k][None, :] == slot_ids for k in range(top)]
    pick = sum(m.astype(F32) for m in match).astype(BF16)

    def exchange(x):
        y = lax.all_to_all(x.reshape(groups, cap, -1), "ep", split_axis=0, concat_axis=0, tiled=True)
        return y.reshape(total, -1)

    w_in = jnp.concatenate([w_gate[0], w_up[0]], axis=1)
    hid = w_gate.shape[2]
    w_mine = lax.dynamic_slice_in_dim(w_in, core * half, half, 0)
    w_other = lax.dynamic_slice_in_dim(w_in, (1 - core) * half, half, 0)
    pre = jnp.dot(rows_in, w_in, preferred_element_type=F32)
    hidden_grad = lax.dot_general(rows_cot, w_down[0], LAST, preferred_element_type=F32)
    gate_pre, up_pre = pre[:, :hid], pre[:, hid:]
    sigma = jax.nn.sigmoid(gate_pre)
    active = gate_pre * sigma
    hidden = (active * up_pre).astype(BF16)
    product_part = jnp.sum(hidden.astype(F32) * hidden_grad, axis=1)
    grads = jnp.concatenate(
        [
            (hidden_grad * up_pre * sigma * (1.0 + gate_pre * (1.0 - sigma))).astype(BF16),
            (hidden_grad * active).astype(BF16),
        ],
        axis=1,
    )
    part_other = lax.dot_general(grads, w_other, LAST, preferred_element_type=F32).astype(BF16)
    arrived = lax.ppermute(part_other, "tp", swap)
    part_mine = lax.dot_general(grads, w_mine, LAST, preferred_element_type=F32)
    row_grads = (part_mine + arrived.astype(F32)).astype(BF16)
    high = product_part.astype(BF16)
    low = (product_part - high.astype(F32)).astype(BF16)
    lane = lax.broadcasted_iota(jnp.int32, (total, 128), 1)
    spare = jnp.where(lane == 0, high[:, None], jnp.where(lane == 1, low[:, None], jnp.zeros((), BF16)))
    row_grads = jnp.concatenate([row_grads, spare], axis=1)
    back = exchange(row_grads)

    rows_in, grads, rows_cot, hidden, row_grads = lax.optimization_barrier(
        (rows_in, grads, rows_cot, hidden, row_grads)
    )
    gate_sum = lax.dot_general(rows_in, grads[:, :hid], ROWS, preferred_element_type=F32)
    up_sum = lax.dot_general(rows_in, grads[:, hid:], ROWS, preferred_element_type=F32)
    down_sum = lax.dot_general(hidden, rows_cot, ROWS, preferred_element_type=F32)
    in_norms = jnp.stack([jnp.sum(gate_sum * gate_sum, axis=1), jnp.sum(up_sum * up_sum, axis=1)])
    down_norms = jnp.sum(down_sum * down_sum, axis=1)
    in_norms = in_norms + lax.ppermute(in_norms, "tp", swap)
    pair = lax.dot_general(
        back[:, half:], jnp.concatenate([match[k] for k in range(top)], axis=1).astype(BF16), ROWS,
        preferred_element_type=F32,
    )
    route_products = (pair[0] + pair[1]).reshape(top, tok_rows)
    route_products = route_products + lax.ppermute(route_products, "tp", swap)
    gate_grad = (route_products.astype(BF16).astype(F32) / gate_t).T
    token_grad = lax.dot_general(pick, back[:, :half], ROWS, preferred_element_type=F32).astype(BF16)
    return (
        token_grad,
        gate_grad,
        gate_sum.astype(BF16)[None],
        up_sum.astype(BF16)[None],
        down_sum.astype(BF16)[None],
        in_norms[0][None],
        in_norms[1][None],
        down_norms[None],
    )


def solution(mesh):
    placed = (
        P("ep", "tp"),
        P("ep", "tp"),
        P("ep", None),
        P("ep", None),
        P("ep", None, "tp"),
        P("ep", None, "tp"),
        P("ep", "tp", None),
    )
    return jax.shard_map(
        per_device,
        mesh=mesh,
        in_specs=placed,
        out_specs=(
            P("ep", "tp"),
            P("ep", None),
            P("ep", None, "tp"),
            P("ep", None, "tp"),
            P("ep", "tp", None),
            P("ep", None),
            P("ep", None),
            P("ep", "tp"),
        ),
        check_vma=False,
    )
```

```python
import functools
import jax
import jax.numpy as jnp
from jax import lax
from jax.experimental import pallas as pl
from jax.experimental.pallas import tpu as pltpu
from jax.sharding import PartitionSpec as P

F32 = jnp.float32
BF16 = jnp.bfloat16
LAST = (((1,), (1,)), ((), ()))
ROWS = (((0,), (0,)), ((), ()))
MESH = pl.DeviceIdType.MESH
VMEM_BYTES = 67043328


def slots_of(routes, groups, cap):
    rows = routes.shape[1]
    ids = lax.broadcasted_iota(jnp.int32, (groups, rows), 0)
    hits = [routes[k][None, :] == ids for k in range(routes.shape[0])]
    named = sum(h.astype(F32) for h in hits).astype(BF16)
    before = (
        lax.broadcasted_iota(jnp.int32, (rows, rows), 0)
        < lax.broadcasted_iota(jnp.int32, (rows, rows), 1)
    ).astype(BF16)
    rank = jnp.dot(named, before, preferred_element_type=F32)
    return jnp.stack(
        [routes[k] * cap + jnp.sum(jnp.where(h, rank, 0.0), axis=0).astype(jnp.int32) for k, h in enumerate(hits)]
    )


def wide(width):
    for step in (512, 384, 256, 128):
        if width % step == 0:
            return step
    return width


def layer_kernel(
    n, cap, tok_ref, cot_ref, meta_ref, w_gate, w_up, w_down,
    tok_out, gate_out, gate_w, up_w, down_w, in_norms, down_norms,
    held, relay, hmeta, rmeta, snd, rows, pick, slot_gate, w_in, w_out, pre, grads, hidden,
    part, arr, back_own, back_far, far_part, prod, norms, col_norm,
    held_send, held_recv, relay_send, relay_recv, meta_sem,
    own_send, own_recv, far_send, far_recv, pair_send, pair_recv, w_sem,
    part_send, part_recv, bo_send, bo_recv, bf_send, bf_recv, fp_send, fp_recv,
    prod_send, prod_recv, pp_sem, norm_sem, out_sem, tok_sem,
):
    rows_t, width = tok_ref.shape
    hid = w_down.shape[1]
    half_n, quarter = n // 2, n // 4
    unit = quarter * cap
    me, core = lax.axis_index("ep"), lax.axis_index("tp")
    plane, xy = me // quarter, me % quarter
    side, spot = me // half_n, me % half_n
    outer = jnp.logical_or(plane == 0, plane == 3)
    inner = jnp.logical_not(outer)
    cross = jnp.where(plane == 1, 2, 1) * quarter + xy
    own_inner = (1 + side) * quarter + xy
    own_base = side * half_n
    near_base = (2 - side) * quarter
    far_base = 3 * (1 - side) * quarter
    bases = (near_base, far_base)
    columns = pl.ds(pl.multiple_of(core * width, width), width)
    source = (tok_ref, cot_ref)
    blocks = half_n * cap
    step = wide(width)
    chunks = width // step
    tiles = hid // 128

    def cols(c):
        return pl.ds(c * step, step)

    def remote(src, dst, send, recv, ep, tp=None):
        return pltpu.make_async_remote_copy(
            src_ref=src, dst_ref=dst, send_sem=send, recv_sem=recv,
            device_id={"ep": ep, "tp": core if tp is None else tp}, device_id_type=MESH,
        )

    loads = []
    for j in range(tiles):
        for k, w in enumerate((w_gate, w_up)):
            loads.append(pltpu.make_async_copy(
                w.at[0, :, pl.ds(j * 128, 128)], w_in.at[:, pl.ds(j * 256 + k * 128, 128)], w_sem.at[len(loads)]
            ))
    loads.append(pltpu.make_async_copy(w_down.at[0], w_out, w_sem.at[len(loads)]))

    barrier = pltpu.get_barrier_semaphore()
    for s in range(1, n):
        pl.semaphore_signal(barrier, inc=1, device_id={"ep": (me + s) % n, "tp": core}, device_id_type=MESH)
    pl.semaphore_signal(barrier, inc=1, device_id={"ep": me, "tp": 1 - core}, device_id_type=MESH)
    pl.semaphore_wait(barrier, n)

    def near_copy(a):
        return remote(source[a], held.at[0, a], held_send.at[0, a], held_recv.at[0, a], cross)

    def relay_copy(a):
        return remote(source[a], relay.at[a], relay_send.at[a], relay_recv.at[a], own_inner)

    def pass_copy(a):
        return remote(relay.at[a], held.at[1, a], held_send.at[1, a], held_recv.at[1, a], cross)

    near_meta = remote(meta_ref, hmeta.at[0], meta_sem.at[0], meta_sem.at[1], cross)
    relay_meta = remote(meta_ref, rmeta, meta_sem.at[2], meta_sem.at[3], own_inner)
    pass_meta = remote(rmeta, hmeta.at[1], meta_sem.at[4], meta_sem.at[5], cross)

    def own_copy(a, s):
        target = (spot + s) % half_n
        return remote(
            snd.at[0, a, target], rows.at[a, me, :, columns],
            own_send.at[a, s], own_recv.at[a, s], own_base + target,
        )

    def far_copy(b, a, s, out):
        target = (xy + s) % quarter
        plane_to = 3 * side if out else 1 + side
        return remote(
            snd.at[1 - b, a, (plane_to % 2) * quarter + target], rows.at[a, bases[b] + xy, :, columns],
            far_send.at[b, a, int(out), s], far_recv.at[b, a, s], plane_to * quarter + target,
        )

    spans = ((own_base, half_n), (near_base, quarter), (far_base, quarter))

    def pair_copy(a, slot):
        block = rows.at[a, pl.ds(*spans[slot]), :, columns]
        return remote(block, block, pair_send.at[a, slot], pair_recv.at[a, slot], me, 1 - core)

    def make_pick(b, table):
        slot = table[0:2, :].astype(jnp.int32) - side * blocks
        ids = lax.broadcasted_iota(jnp.int32, (blocks, rows_t), 0)
        match = [slot[k:k + 1, :] == ids for k in range(2)]
        pick[b] = sum(m.astype(F32) for m in match).astype(BF16)
        slot_gate[b] = sum(
            jnp.sum(jnp.where(m, table[2 + k:3 + k, :], 0.0), axis=1, keepdims=True) for k, m in enumerate(match)
        )

    def fill(b, where, a, src):
        @pl.loop(0, chunks)
        def _(c):
            span = pl.ds(pl.multiple_of(c * step, step), step)
            block = jnp.dot(pick[b], src[:, span], preferred_element_type=F32)
            if a == 1:
                block = block * slot_gate[b]
            snd[where, a, :, :, span] = block.astype(BF16).reshape(half_n, cap, step)

    def hand_on(b, a):
        fill(1 + b, 1 - b, a, held.at[b, a])
        for s in range(quarter):
            far_copy(b, a, s, True).start()
        for s in range(1, quarter):
            far_copy(b, a, s, False).start()
        rows[a, bases[b] + xy, :, columns] = snd[1 - b, a, (1 - side) * quarter + xy]

    def own_arrived(a):
        for s in range(1, half_n):
            own_copy(a, s).wait_recv()
        pair_copy(a, 0).start()

    def far_arrived(b, a):
        for s in range(1, quarter):
            far_copy(b, a, s, False).wait_recv()

        @pl.when(outer)
        def _():
            far_copy(b, a, 0, True).wait_recv()

        pair_copy(a, 1 + b).start()

    def pre_unit(base):
        x = rows[0, pl.ds(base, quarter)].reshape(unit, 2 * width)
        pre[pl.ds(base, quarter)] = jnp.dot(x, w_in[...], preferred_element_type=F32).reshape(quarter, cap, 2 * hid)

    def mid_unit(base):
        x = rows[1, pl.ds(base, quarter)].reshape(unit, 2 * width)
        grad = lax.dot_general(x, w_out[...], LAST, preferred_element_type=F32)
        total = jnp.zeros((unit, 1), F32)
        for j in range(tiles):
            gate_pre = pre[pl.ds(base, quarter), :, j * 256:j * 256 + 128].reshape(unit, 128)
            up_pre = pre[pl.ds(base, quarter), :, j * 256 + 128:j * 256 + 256].reshape(unit, 128)
            g = grad[:, j * 128:(j + 1) * 128]
            sigma = jax.nn.sigmoid(gate_pre)
            active = gate_pre * sigma
            kept = (active * up_pre).astype(BF16)
            total = total + jnp.sum(kept.astype(F32) * g, axis=1, keepdims=True)
            hidden[pl.ds(base, quarter), :, j * 128:(j + 1) * 128] = kept.reshape(quarter, cap, 128)
            one = (g * up_pre * sigma * (1.0 + gate_pre * (1.0 - sigma))).astype(BF16)
            two = (g * active).astype(BF16)
            grads[pl.ds(base, quarter), :, j * 256:j * 256 + 128] = one.reshape(quarter, cap, 128)
            grads[pl.ds(base, quarter), :, j * 256 + 128:j * 256 + 256] = two.reshape(quarter, cap, 128)
        diagonal = lax.broadcasted_iota(jnp.int32, (cap, 128), 0) == lax.broadcasted_iota(jnp.int32, (cap, 128), 1)
        for q in range(quarter):
            line = jnp.sum(jnp.where(diagonal, total[q * cap:(q + 1) * cap], 0.0), axis=0, keepdims=True)
            prod[0, base + q] = jnp.broadcast_to(line, (8, 128))

    def part_copy(kind, c):
        block = pl.ds(*spans[kind])
        return remote(
            part.at[block, :, cols(c)], arr.at[block, :, cols(c)],
            part_send.at[kind, c], part_recv.at[kind, c], me, 1 - core,
        )

    def product(base, c, whose):
        g = grads[pl.ds(base, quarter)].reshape(unit, 2 * hid)
        w = w_in[pl.ds(pl.multiple_of(whose * width + c * step, step), step), :]
        return lax.dot_general(g, w, LAST, preferred_element_type=F32).reshape(quarter, cap, step)

    def unit_bases(kind):
        return (own_base, own_base + quarter) if kind == 0 else (bases[kind - 1],)

    def part_out(kind):
        for c in range(chunks):
            for base in unit_bases(kind):
                part[pl.ds(base, quarter), :, cols(c)] = product(base, c, 1 - core).astype(BF16)
            part_copy(kind, c).start()

    def back_own_copy(c, s):
        target = (spot + s) % half_n
        return remote(
            arr.at[own_base + target, :, cols(c)], back_own.at[spot, :, cols(c)],
            bo_send.at[c, s], bo_recv.at[c, spot], own_base + target,
        )

    def back_far_copy(b, c, s):
        target = (xy + s) % quarter
        return remote(
            arr.at[bases[b] + target, :, cols(c)], back_far.at[b, spot, :, cols(c)],
            bf_send.at[b, c, s], bf_recv.at[b, c, spot], (1 + side) * quarter + target,
        )

    def send_back(kind):
        for c in range(chunks):
            part_copy(kind, c).wait_recv()
            for base in unit_bases(kind):
                here = pl.ds(base, quarter)
                arr[here, :, cols(c)] = (product(base, c, core) + arr[here, :, cols(c)].astype(F32)).astype(BF16)
            if kind == 0:
                for s in range(1, half_n):
                    back_own_copy(c, s).start()
                back_own[spot, :, cols(c)] = arr[me, :, cols(c)]
            else:
                for s in range(1, quarter):
                    back_far_copy(kind - 1, c, s).start()

                @pl.when(outer)
                def _():
                    back_far_copy(kind - 1, c, 0).start()

                @pl.when(inner)
                def _():
                    back_far[kind - 1, spot, :, cols(c)] = arr[bases[kind - 1] + xy, :, cols(c)]

    def far_part_copy(b, c):
        return remote(
            relay.at[b, :, cols(c)], far_part.at[:, cols(c)],
            fp_send.at[b, c], fp_recv.at[c], cross if b == 0 else far_base + xy,
        )

    def combine(b, src, c):
        block = src[:, :, cols(c)].reshape(blocks, step)
        return lax.dot_general(pick[b], block, ROWS, preferred_element_type=F32)

    def far_combine(b):
        for c in range(chunks):
            for s in range(1, half_n):
                other = (spot + s) % half_n
                block = back_far.at[b, other, :, cols(c)]
                remote(block, block, bf_send.at[b, c, 0], bf_recv.at[b, c, other], me, 1 - core).wait_recv()
            relay[b, :, cols(c)] = combine(1 + b, back_far.at[b], c).astype(BF16)
            far_part_copy(b, c).start()

    @pl.when(inner)
    def _():
        near_meta.start()
        near_copy(0).start()
        near_copy(1).start()

    @pl.when(outer)
    def _():
        relay_meta.start()
        relay_copy(0).start()

    for load in loads:
        load.start()
    make_pick(0, meta_ref)
    for a in range(2):
        if a == 1:
            @pl.when(outer)
            def _():
                relay_copy(1).start()
        fill(0, 0, a, source[a])
        for s in range(half_n - 1, 0, -1):
            own_copy(a, s).start()
        rows[a, me, :, columns] = snd[0, a, spot]

    @pl.when(inner)
    def _():
        near_meta.wait_recv()
        relay_meta.wait_recv()
        pass_meta.start()
        make_pick(1, hmeta.at[0])
        relay_copy(0).wait_recv()
        pass_copy(0).start()
        near_copy(0).wait_recv()
        hand_on(0, 0)

    own_arrived(0)

    @pl.when(inner)
    def _():
        near_copy(1).wait_recv()
        hand_on(0, 1)

    far_arrived(0, 0)
    for load in loads:
        load.wait()
    pair_copy(0, 0).wait_recv()

    @pl.loop(0, 2)
    def _(u):
        pre_unit(own_base + u * quarter)

    @pl.when(inner)
    def _():
        pass_meta.wait_recv()
        make_pick(2, hmeta.at[1])
        relay_copy(1).wait_recv()
        pass_copy(1).start()

    pair_copy(0, 1).wait_recv()
    pre_unit(near_base)
    for a in range(2):
        for s in range(1, half_n):
            own_copy(a, s).wait_send()

    @pl.when(inner)
    def _():
        pass_copy(0).wait_recv()
        hand_on(1, 0)

    far_arrived(0, 1)
    pair_copy(1, 1).wait_recv()
    mid_unit(near_base)
    part_out(1)
    own_arrived(1)
    send_back(1)
    pair_copy(1, 0).wait_recv()

    @pl.loop(0, 2)
    def _(u):
        mid_unit(own_base + u * quarter)

    @pl.when(inner)
    def _():
        pass_copy(1).wait_recv()
        hand_on(1, 1)

    far_arrived(1, 0)
    part_out(0)
    pair_copy(0, 2).wait_recv()
    pre_unit(far_base)
    send_back(0)

    @pl.when(inner)
    def _():
        for a in range(2):
            pass_copy(a).wait_send()
        far_combine(0)

    far_arrived(1, 1)
    pair_copy(1, 2).wait_recv()
    mid_unit(far_base)
    part_out(2)
    prod_pair = remote(prod.at[0], prod.at[1], pp_sem.at[0], pp_sem.at[1], me, 1 - core)
    prod_pair.start()
    send_back(2)
    prod_pair.wait()

    def prod_copy(s):
        target = (me + s) % n
        return remote(prod.at[0, target], prod.at[2, me], prod_send.at[s], prod_recv.at[s], target)

    prod[0] = (prod[0] + prod[1]).astype(BF16).astype(F32)
    for s in range(1, n):
        prod_copy(s).start()
    prod[2, me] = prod[0, me]

    eye = lax.broadcasted_iota(jnp.int32, (128, 128), 0) == lax.broadcasted_iota(jnp.int32, (128, 128), 1)

    def lay(column):
        return jnp.sum(jnp.where(eye, column, 0.0), axis=0, keepdims=True)

    @pl.loop(0, 2 * width // 128)
    def _(d):
        span = pl.ds(pl.multiple_of(d * 128, 128), 128)
        x = rows[0, :, :, span].reshape(n * cap, 128)
        sums = lax.dot_general(x, grads[...].reshape(n * cap, 2 * hid), ROWS, preferred_element_type=F32)
        w_in[span, :] = sums.astype(BF16)
        square = sums * sums
        for k in range(2):
            column = sum(
                jnp.sum(square[:, j * 256 + k * 128:j * 256 + k * 128 + 128], axis=1, keepdims=True)
                for j in range(tiles)
            )
            norms[0, k:k + 1, span] = lay(column)

    norm_pair = remote(norms.at[0], norms.at[1], norm_sem.at[0], norm_sem.at[1], me, 1 - core)
    norm_pair.start()
    outs = []
    for j in range(tiles):
        for k, w in enumerate((gate_w, up_w)):
            outs.append(pltpu.make_async_copy(
                w_in.at[:, pl.ds(j * 256 + k * 128, 128)], w.at[0, :, pl.ds(j * 128, 128)], out_sem.at[len(outs)]
            ))
    for out in outs:
        out.start()

    @pl.when(inner)
    def _():
        far_combine(1)

    col_norm[...] = jnp.zeros_like(col_norm)

    @pl.loop(0, 2 * width // step)
    def _(d):
        span = pl.ds(pl.multiple_of(d * step, step), step)
        x = rows[1, :, :, span].reshape(n * cap, step)
        sums = lax.dot_general(
            hidden[...].reshape(n * cap, hid), x, ROWS, preferred_element_type=F32
        )
        w_out[:, span] = sums.astype(BF16)
        col_norm[...] += jnp.sum(sums * sums, axis=1, keepdims=True)

    last = pltpu.make_async_copy(w_out, down_w.at[0], out_sem.at[2 * tiles])
    last.start()
    for j in range(tiles):
        down_norms[:, pl.ds(j * 128, 128)] = jnp.broadcast_to(lay(col_norm[j * 128:(j + 1) * 128]), (8, 128))
    norm_pair.wait()
    in_norms[...] = norms[0] + norms[1]

    for s in range(1, n):
        prod_copy(s).wait_recv()
    table = prod[2][:, 0, :].astype(BF16)
    ids = lax.broadcasted_iota(jnp.int32, (n, rows_t), 0)
    lanes = lax.broadcasted_iota(jnp.int32, (128, rows_t), 0)
    gate_out[...] = jnp.zeros_like(gate_out)
    for k in range(2):
        hit = (meta_ref[4 + k:5 + k, :].astype(jnp.int32) == ids).astype(F32).astype(BF16)
        found = lax.dot_general(table, hit, ROWS, preferred_element_type=F32)
        rank = meta_ref[6 + k:7 + k, :].astype(jnp.int32)
        value = jnp.sum(jnp.where(rank == lanes, found, 0.0), axis=0, keepdims=True)
        gate_out[k:k + 1, :] = value / meta_ref[2 + k:3 + k, :]

    tok_done = []
    for c in range(chunks):
        for s in range(1, half_n):
            other = (spot + s) % half_n
            block = back_own.at[other, :, cols(c)]
            remote(block, block, bo_send.at[c, 0], bo_recv.at[c, other], me, 1 - core).wait_recv()
        mine = combine(0, back_own, c)
        far_part_copy(0, c).wait_recv()
        held[0, 0, :, cols(c)] = (mine + far_part[:, cols(c)].astype(F32)).astype(BF16)
        done = pltpu.make_async_copy(held.at[0, 0, :, cols(c)], tok_out.at[:, cols(c)], tok_sem.at[c])
        done.start()
        tok_done.append(done)

    for a in range(2):
        for slot in range(3):
            pair_copy(a, slot).wait_send()
    for c in range(chunks):
        for kind in range(3):
            part_copy(kind, c).wait_send()
        for s in range(1, half_n):
            back_own_copy(c, s).wait_send()
        for b in range(2):
            for s in range(1, quarter):
                back_far_copy(b, c, s).wait_send()
    for s in range(1, n):
        prod_copy(s).wait_send()

    @pl.when(inner)
    def _():
        near_meta.wait_send()
        pass_meta.wait_send()
        for a in range(2):
            near_copy(a).wait_send()
            for b in range(2):
                for s in range(quarter):
                    far_copy(b, a, s, True).wait_send()
                for s in range(1, quarter):
                    far_copy(b, a, s, False).wait_send()
        for c in range(chunks):
            for b in range(2):
                far_part_copy(b, c).wait_send()

    @pl.when(outer)
    def _():
        relay_meta.wait_send()
        for a in range(2):
            relay_copy(a).wait_send()
        for c in range(chunks):
            for b in range(2):
                back_far_copy(b, c, 0).wait_send()

    for done in tok_done:
        done.wait()
    for out in outs:
        out.wait()
    last.wait()


def scratch(n, cap, rows_t, width, hid):
    half_n, quarter = n // 2, n // 4
    chunks = width // wide(width)
    dma = pltpu.SemaphoreType.DMA
    buffers = [
        ((2, 2, rows_t, width), BF16),
        ((2, rows_t, width), BF16),
        ((2, 8, rows_t), F32),
        ((8, rows_t), F32),
        ((2, 2, half_n, cap, width), BF16),
        ((2, n, cap, 2 * width), BF16),
        ((3, half_n * cap, rows_t), BF16),
        ((3, half_n * cap, 1), F32),
        ((2 * width, 2 * hid), BF16),
        ((hid, 2 * width), BF16),
        ((n, cap, 2 * hid), F32),
        ((n, cap, 2 * hid), BF16),
        ((n, cap, hid), BF16),
        ((n, cap, width), BF16),
        ((n, cap, width), BF16),
        ((half_n, cap, width), BF16),
        ((2, half_n, cap, width), BF16),
        ((rows_t, width), BF16),
        ((3, n, 8, 128), F32),
        ((2, 8, 2 * width), F32),
        ((hid, 1), F32),
    ]
    semaphores = [
        (2, 2), (2, 2), (2,), (2,), (6,),
        (2, half_n), (2, half_n), (2, 2, 2, quarter), (2, 2, quarter), (2, 3), (2, 3), (2 * hid // 128 + 1,),
        (3, chunks), (3, chunks), (chunks, half_n), (chunks, half_n), (2, chunks, quarter), (2, chunks, half_n),
        (2, chunks), (chunks,), (n,), (n,), (2,), (2,), (2 * hid // 128 + 1,), (chunks,),
    ]
    size = 2 * rows_t * width * 2
    for shape, kind in buffers:
        lanes = -(-shape[-1] // 128) * 128
        count = lanes
        for extent in shape[:-1]:
            count *= extent
        size += count * (2 if kind == BF16 else 4)
    return [pltpu.VMEM(*b) for b in buffers] + [dma(s) for s in semaphores], size


def fused(n, cap, tokens, cotangent, meta, w_gate, w_up, w_down):
    rows_t, width = tokens.shape
    hid = w_down.shape[1]
    vm = pl.BlockSpec(memory_space=pltpu.VMEM)
    anywhere = pl.BlockSpec(memory_space=pl.ANY)
    shape = jax.ShapeDtypeStruct
    return pl.pallas_call(
        functools.partial(layer_kernel, n, cap),
        out_shape=(
            shape(tokens.shape, BF16), shape((8, rows_t), F32),
            shape(w_gate.shape, BF16), shape(w_up.shape, BF16), shape(w_down.shape, BF16),
            shape((8, 2 * width), F32), shape((8, hid), F32),
        ),
        in_specs=[vm] * 3 + [anywhere] * 3,
        out_specs=[anywhere, vm, anywhere, anywhere, anywhere, vm, vm],
        scratch_shapes=scratch(n, cap, rows_t, width, hid)[0],
        compiler_params=pltpu.CompilerParams(
            collective_id=0, has_side_effects=True, vmem_limit_bytes=VMEM_BYTES
        ),
        cost_estimate=pl.CostEstimate(flops=10**10, bytes_accessed=10**8, transcendentals=0),
    )(tokens, cotangent, meta, w_gate, w_up, w_down)


def per_device(tokens, cotangent, experts, gate, w_gate, w_up, w_down):
    groups = lax.axis_size("ep")
    tok_rows, top = experts.shape
    cap = 3 * tok_rows * top // (2 * groups)
    cap = (cap + 7) // 8 * 8
    slot = slots_of(experts.T, groups, cap)
    gate_t = gate.T
    rank = slot - experts.T * cap
    meta = jnp.concatenate([slot.astype(F32), gate_t, experts.T.astype(F32), rank.astype(F32)], axis=0)
    tok, gate_grad, gate_w, up_w, down_w, in_norms, down_norms = fused(
        groups, cap, tokens, cotangent, meta, w_gate, w_up, w_down
    )
    return (
        tok, gate_grad[:top].T, gate_w, up_w, down_w, in_norms[0][None], in_norms[1][None], down_norms[0][None],
    )


def plain_device(tokens, cotangent, experts, gate, w_gate, w_up, w_down):
    groups = lax.axis_size("ep")
    tok_rows, top = experts.shape
    cap = 3 * tok_rows * top // (2 * groups)
    total = groups * cap
    half = tokens.shape[1]
    core = lax.axis_index("tp")
    swap = [(0, 1), (1, 0)]
    slot = slots_of(experts.T, groups, cap)
    gate_t = gate.T
    slot_ids = lax.broadcasted_iota(jnp.int32, (total, tok_rows), 0)
    match = [slot[k][None, :] == slot_ids for k in range(top)]
    pick = sum(m.astype(F32) for m in match).astype(BF16)
    slot_gate = sum(
        jnp.sum(jnp.where(m, gate_t[k][None, :], 0.0), axis=1, keepdims=True) for k, m in enumerate(match)
    )
    pick, slot_gate = lax.optimization_barrier((pick, slot_gate))

    def exchange(x):
        y = lax.all_to_all(x.reshape(groups, cap, -1), "ep", split_axis=0, concat_axis=0, tiled=True)
        return y.reshape(total, -1)

    sent_tok = jnp.dot(pick, tokens, preferred_element_type=F32).astype(BF16)
    own_tok = exchange(sent_tok)
    cot = jnp.dot(pick, cotangent, preferred_element_type=F32)
    sent_cot = (cot * slot_gate).astype(BF16)
    own_cot = exchange(sent_cot)

    def both(own, other):
        return jnp.where(
            core == 0,
            jnp.concatenate([own, other], axis=1),
            jnp.concatenate([other, own], axis=1),
        )

    w_in = jnp.concatenate([w_gate[0], w_up[0]], axis=1)
    hid = w_gate.shape[2]
    w_mine = lax.dynamic_slice_in_dim(w_in, core * half, half, 0)
    w_other = lax.dynamic_slice_in_dim(w_in, (1 - core) * half, half, 0)
    d_mine = lax.dynamic_slice_in_dim(w_down[0], core * half, half, 1)
    d_other = lax.dynamic_slice_in_dim(w_down[0], (1 - core) * half, half, 1)

    other_tok = lax.ppermute(own_tok, "tp", swap)
    rows_in = both(own_tok, other_tok)
    pre = jnp.dot(rows_in, w_in, preferred_element_type=F32)
    other_cot = lax.ppermute(own_cot, "tp", swap)
    grad_mine = lax.dot_general(own_cot, d_mine, LAST, preferred_element_type=F32)
    hidden_grad = grad_mine + lax.dot_general(other_cot, d_other, LAST, preferred_element_type=F32)
    gate_pre, up_pre = pre[:, :hid], pre[:, hid:]
    sigma = jax.nn.sigmoid(gate_pre)
    active = gate_pre * sigma
    hidden = (active * up_pre).astype(BF16)
    product_part = jnp.sum(hidden.astype(F32) * hidden_grad, axis=1)
    grads = jnp.concatenate(
        [
            (hidden_grad * up_pre * sigma * (1.0 + gate_pre * (1.0 - sigma))).astype(BF16),
            (hidden_grad * active).astype(BF16),
        ],
        axis=1,
    )
    part_other = lax.dot_general(grads, w_other, LAST, preferred_element_type=F32).astype(BF16)
    arrived = lax.ppermute(part_other, "tp", swap)
    part_mine = lax.dot_general(grads, w_mine, LAST, preferred_element_type=F32)
    row_grads = (part_mine + arrived.astype(F32)).astype(BF16)
    high = product_part.astype(BF16)
    low = (product_part - high.astype(F32)).astype(BF16)
    lane = lax.broadcasted_iota(jnp.int32, (total, 128), 1)
    spare = jnp.where(lane == 0, high[:, None], jnp.where(lane == 1, low[:, None], jnp.zeros((), BF16)))
    row_grads = jnp.concatenate([row_grads, spare], axis=1)
    back = exchange(row_grads)

    rows_in, grads, other_cot, hidden, row_grads = lax.optimization_barrier(
        (rows_in, grads, other_cot, hidden, row_grads)
    )
    gate_sum = lax.dot_general(rows_in, grads[:, :hid], ROWS, preferred_element_type=F32)
    up_sum = lax.dot_general(rows_in, grads[:, hid:], ROWS, preferred_element_type=F32)
    rows_cot = both(own_cot, other_cot)
    down_sum = lax.dot_general(hidden, rows_cot, ROWS, preferred_element_type=F32)
    in_norms = jnp.stack([jnp.sum(gate_sum * gate_sum, axis=1), jnp.sum(up_sum * up_sum, axis=1)])
    down_norms = jnp.sum(down_sum * down_sum, axis=1)
    in_norms = in_norms + lax.ppermute(in_norms, "tp", swap)
    pair = lax.dot_general(
        back[:, half:], jnp.concatenate([match[k] for k in range(top)], axis=1).astype(BF16), ROWS,
        preferred_element_type=F32,
    )
    route_products = (pair[0] + pair[1]).reshape(top, tok_rows)
    route_products = route_products + lax.ppermute(route_products, "tp", swap)
    gate_grad = (route_products.astype(BF16).astype(F32) / gate_t).T
    token_grad = lax.dot_general(pick, back[:, :half], ROWS, preferred_element_type=F32).astype(BF16)
    return (
        token_grad,
        gate_grad,
        gate_sum.astype(BF16)[None],
        up_sum.astype(BF16)[None],
        down_sum.astype(BF16)[None],
        in_norms[0][None],
        in_norms[1][None],
        down_norms[None],
    )


def layer(run, *arrays):
    return run(*arrays)


def fits(n, cores, shapes):
    tokens, experts, w_down = shapes
    rows_t, top = experts[0] // n, experts[1]
    cap = (3 * rows_t * top // (2 * n) + 7) // 8 * 8
    width, hid = tokens[1] // cores, w_down[1] // cores
    if n % 4 or cores != 2 or top != 2 or hid % 128 or width % 128 or cap > 128 or w_down[0] != n:
        return False
    return scratch(n, cap, rows_t, width, hid)[1] < VMEM_BYTES


def solution(mesh):
    placed = (
        P("ep", "tp"),
        P("ep", "tp"),
        P("ep", None),
        P("ep", None),
        P("ep", None, "tp"),
        P("ep", None, "tp"),
        P("ep", "tp", None),
    )

    def mapped(run):
        return jax.shard_map(
            functools.partial(layer, run),
            mesh=mesh,
            in_specs=placed,
            out_specs=(
                P("ep", "tp"),
                P("ep", None),
                P("ep", None, "tp"),
                P("ep", None, "tp"),
                P("ep", "tp", None),
                P("ep", None),
                P("ep", None),
                P("ep", "tp"),
            ),
            check_vma=False,
        )

    plain = mapped(plain_device)
    quick = mapped(per_device)

    def run(*arrays):
        shapes = (arrays[0].shape, arrays[2].shape, arrays[6].shape)
        return (quick if fits(mesh.shape["ep"], mesh.shape["tp"], shapes) else plain)(*arrays)

    return run
```
